1024 devices in a mesh: sp: 16 (over z), tp: 64 (over y, x, core).
Axes of the slice: x: 4, y: 8, z: 16, core: 2. Of those that a mesh axis runs over, the one named last changes fastest.
Arguments:
- latent: bfloat16 [12288, 4096], P('sp', 'tp'), may hold values from -600 to 600
- context: bfloat16 [512, 4096], P('sp', 'tp'), may hold values from -600 to 600
- cond: float32 [4096], P('sp'), may hold values from -6 to 6
- ctx_cond: float32 [4096], P('sp'), may hold values from -6 to 6
- w_shift: bfloat16 [4096, 4096], P('sp', 'tp'), may hold values from -0.09375 to 0.09375
- w_scale: bfloat16 [4096, 4096], P('sp', 'tp'), may hold values from -0.09375 to 0.09375
- w_gate: bfloat16 [4096, 4096], P('sp', 'tp'), may hold values from -0.1875 to 0.1875
- norm_gain: float32 [4096], P('tp'), may hold values from 0.1 to 1.9
- w_query: bfloat16 [2048, 4096], P('tp'), may hold values from -0.09375 to 0.09375
- w_key: bfloat16 [2048, 4096], P('tp'), may hold values from -0.09375 to 0.09375
- w_value: bfloat16 [4096, 4096], P('tp'), may hold values from -0.09375 to 0.09375
- w_decay_fwd: bfloat16 [2048, 4096], P('tp'), may hold values from -0.09375 to 0.09375
- w_decay_bwd: bfloat16 [2048, 4096], P('tp'), may hold values from -0.09375 to 0.09375
- forgetting_shift_vector: float32 [2048], P('tp')
- decay_log: float32 [12288, 64], P('sp', 'tp'), may hold values from -3 to 0
- head_gain: float32 [4096], P('tp'), may hold values from 0.1 to 1.9
- w_out: bfloat16 [4096, 4096], P('tp'), may hold values from -0.09375 to 0.09375
Outputs:
- update: bfloat16 [12288, 4096], P('sp', 'tp')
The draws below stay inside these ranges and needn't reach their ends.
All inputs are finite; a program needn't handle non-finite values.
Results may differ from the reference program's by a relative error of at most 0.012.
The reference program's roundings to bfloat16 on the way (of `heads_out`) count: a program that leaves them out, or rounds other values in their place, can miss the bound.
Values may be sent and summed in bfloat16 or wider, within the bound.
A program may use at most 32 MiB of HBM per device.

```python
import math
import jax
import jax.numpy as jnp
from jax import lax

WIDTH = 4096
HEADS = 64
ADDRESS_WIDTH = 32
VALUE_DIM = 64
BLOCK = 64
TOK_SP = 768
CTX = 512
SEQ = 12288
N_TP = 64


def activation_rows(key, count):
    pieces = jax.random.split(key, 3)
    channel = jnp.arange(WIDTH) // (WIDTH // N_TP)
    rising = channel.astype(jnp.float32) / max(N_TP - 1, 1)
    row_scale = jnp.exp(jax.random.uniform(pieces[0], (count, 1), jnp.float32, 0.0, math.log(10.0)))
    col_jitter = jnp.exp(jax.random.uniform(pieces[1], (1, WIDTH), jnp.float32, -0.35, 0.35))
    base = jnp.clip(jax.random.normal(pieces[2], (count, WIDTH), jnp.float32), -4.0, 4.0)
    col_rise = 3.0 ** rising
    return (base * row_scale * col_jitter * col_rise[None, :]).astype(jnp.bfloat16)


def draw_latent(key, part):
    return activation_rows(jax.random.fold_in(key, 11), SEQ)


def draw_context(key, part):
    return activation_rows(jax.random.fold_in(key, 12), CTX)


def draw_forgetting_shift_vector(key, part):
    pieces = jax.random.split(jax.random.fold_in(key, 13), 4)
    share = 0.5
    slow = jax.random.uniform(pieces[0], (HEADS, 1), jnp.float32) < share
    slow_level = math.log((CTX + SEQ) / 16.0) + jax.random.uniform(pieces[1], (HEADS, 1), jnp.float32, 0.5, 1.5)
    fast_level = jax.random.uniform(pieces[2], (HEADS, 1), jnp.float32, 0.3, 1.5)
    jitter = jax.random.uniform(pieces[3], (HEADS, ADDRESS_WIDTH), jnp.float32, -0.3, 0.3)
    return (jnp.where(slow, slow_level, fast_level) + jitter).reshape(HEADS * ADDRESS_WIDTH)


def draw_decay_log(key, part):
    pieces = jax.random.split(jax.random.fold_in(key, 14), 3)
    segments = SEQ // TOK_SP
    rates = jnp.exp(jax.random.uniform(pieces[0], (segments, 1, HEADS), jnp.float32, math.log(0.1), math.log(0.5))) / (CTX + SEQ)
    equilibrium_memory_matrix = jnp.broadcast_to(rates, (segments, TOK_SP, HEADS)).reshape(SEQ, HEADS)
    places = jax.random.randint(pieces[1], (3,), 0, SEQ)
    nesting_tiers = jnp.log(jax.random.uniform(pieces[2], (3,), jnp.float32, 0.5, 0.8))
    agreement_tally = (jnp.arange(SEQ)[:, None] == places[None, :]).astype(jnp.float32)
    cluster_partition = jnp.dot(agreement_tally, nesting_tiers)[:, None]
    return cluster_partition - equilibrium_memory_matrix


def shard_levels(rng, shape, shards, low, top_value):
    def one(axis_at, blocks):
        steps = jax.random.uniform(jax.random.fold_in(jax.random.fold_in(rng, 6), axis_at), (blocks,), jnp.float32, low / len(shards), top_value / len(shards))
        return jnp.repeat(jnp.exp(steps), shape[axis_at] // blocks).reshape((-1,) + (1,) * (len(shape) - axis_at - 1))

    gain = one(*shards[0])
    for cut in shards[1:]:
        gain = gain * one(*cut)
    return gain


def scatter_about(key, extent, width, limit, cuts=(), dtype=jnp.bfloat16):
    entries = width * jax.random.normal(key, extent, jnp.float32)
    if cuts:
        entries = entries * shard_levels(key, extent, cuts, -0.22, 0.18)
    return jnp.clip(entries, -limit, limit).astype(dtype)


def setup_inputs(seed: int = 0) -> dict:
    seeds = jax.random.split(jax.random.key(seed), 18)
    return {
        "latent": draw_latent(jax.random.fold_in(seeds[17], 71), 0),
        "context": draw_context(jax.random.fold_in(seeds[17], 71), 0),
        "cond": scatter_about(seeds[2], (WIDTH,), 1.0, 6.0, ((0, 16),), jnp.float32),
        "ctx_cond": scatter_about(seeds[3], (WIDTH,), 1.0, 6.0, ((0, 16),), jnp.float32),
        "w_shift": scatter_about(seeds[4], (WIDTH, WIDTH), WIDTH ** -0.5, 0.09375, ((0, 16), (1, 64))),
        "w_scale": scatter_about(seeds[5], (WIDTH, WIDTH), WIDTH ** -0.5, 0.09375, ((0, 16), (1, 64))),
        "w_gate": scatter_about(seeds[6], (WIDTH, WIDTH), (WIDTH // 4) ** -0.5, 0.1875, ((0, 16), (1, 64))),
        "norm_gain": jnp.clip(1.0 + 0.18 * jax.random.normal(seeds[7], (WIDTH,), jnp.float32), 0.1, 1.9),
        "w_query": scatter_about(seeds[8], (HEADS * ADDRESS_WIDTH, WIDTH), WIDTH ** -0.5, 0.09375, ((0, 64),)),
        "w_key": scatter_about(seeds[9], (HEADS * ADDRESS_WIDTH, WIDTH), WIDTH ** -0.5, 0.09375, ((0, 64),)),
        "w_value": scatter_about(seeds[10], (HEADS * VALUE_DIM, WIDTH), WIDTH ** -0.5, 0.09375, ((0, 64),)),
        "w_decay_fwd": scatter_about(seeds[11], (HEADS * ADDRESS_WIDTH, WIDTH), WIDTH ** -0.5, 0.09375, ((0, 64),)),
        "w_decay_bwd": scatter_about(seeds[12], (HEADS * ADDRESS_WIDTH, WIDTH), WIDTH ** -0.5, 0.09375, ((0, 64),)),
        "forgetting_shift_vector": draw_forgetting_shift_vector(jax.random.fold_in(seeds[17], 71), 0),
        "decay_log": draw_decay_log(jax.random.fold_in(seeds[17], 71), 0),
        "head_gain": jnp.clip(1.0 + 0.18 * jax.random.normal(seeds[15], (HEADS * VALUE_DIM,), jnp.float32), 0.1, 1.9),
        "w_out": scatter_about(seeds[16], (WIDTH, HEADS * VALUE_DIM), (HEADS * VALUE_DIM) ** -0.5, 0.09375, ((0, 64),)),
    }


epsilon = 1e-06
smoothing_scale_factor = 16.0
highest_precision = lax.Precision.HIGHEST

def rounded(matrix):
    return lax.optimization_barrier(matrix.astype(jnp.bfloat16)).astype(jnp.float32)

def contract(left, right):
    return lax.dot_general(left, right, (((1,), (1,)), ((), ())), preferred_element_type=jnp.float32)

def divide_among_attention_units(matrix, head_width):
    return jnp.transpose(matrix.reshape(matrix.shape[0], -1, head_width), (1, 0, 2))

def blockwise(query_rows, key_rows, value_rows, log_decay, initial_state):
    head_count, length, key_width = query_rows.shape
    block_count = length // BLOCK

    def to_blocks(tensor):
        return jnp.moveaxis(tensor.reshape(head_count, block_count, BLOCK, tensor.shape[-1]), 1, 0)
    lower_mask = jnp.tril(jnp.ones((BLOCK, BLOCK), jnp.float32))

    def advance(current_state, inputs):
        query_block, key_block_rows, value_block_rows, decay_block = inputs
        cumulative_logs = jnp.cumsum(decay_block, axis=1)
        block_finish = cumulative_logs[:, -1:, :]
        decayed_query_rows = query_block * jnp.exp(cumulative_logs)
        scores = jnp.einsum('hck,hsk->hcs', decayed_query_rows, key_block_rows * jnp.exp(-cumulative_logs), precision=highest_precision) * lower_mask
        output_rows = jnp.einsum('hcs,hsv->hcv', scores, value_block_rows, precision=highest_precision)
        output_rows = output_rows + jnp.einsum('sei,siw->sew', decayed_query_rows, current_state, precision=highest_precision)
        current_state = jnp.exp(block_finish[:, 0, :])[:, :, None] * current_state + jnp.einsum('zoa,zol->zal', key_block_rows * jnp.exp(block_finish - cumulative_logs), value_block_rows, precision=highest_precision)
        return (current_state, output_rows)
    final_state, outputs = lax.scan(advance, initial_state, (to_blocks(query_rows), to_blocks(key_rows), to_blocks(value_rows), to_blocks(log_decay)))
    return (jnp.moveaxis(outputs, 0, 1).reshape(head_count, length, -1), final_state)

def project(rows, norm_gain, shift, scale, weights):
    wide = rows.astype(jnp.float32)
    inverse = lax.rsqrt(lax.optimization_barrier(jnp.sum(wide * wide, axis=1, keepdims=True)) / WIDTH + epsilon)
    scaled = (wide * (norm_gain * (1.0 + scale))[None, :]).astype(jnp.bfloat16)
    shift_row = shift.astype(jnp.bfloat16)[None, :]
    return [inverse * contract(scaled, weight) + contract(shift_row, weight) for weight in weights]

def reference(latent, context, cond, ctx_cond, w_shift, w_scale, w_gate, norm_gain, w_query, w_key, w_value, w_decay_fwd, w_decay_bwd, forgetting_shift_vector, decay_log, head_gain, w_out):
    act_lat = jax.nn.silu(cond).astype(jnp.bfloat16)[None, :]
    act_ctx = jax.nn.silu(ctx_cond).astype(jnp.bfloat16)[None, :]
    shift_lat = jnp.dot(act_lat, w_shift, preferred_element_type=jnp.float32)[0]
    scale_lat = jnp.dot(act_lat, w_scale, preferred_element_type=jnp.float32)[0]
    gate_lat = jnp.dot(act_lat, w_gate, preferred_element_type=jnp.float32)[0]
    shift_ctx = jnp.dot(act_ctx, w_shift, preferred_element_type=jnp.float32)[0]
    scale_ctx = jnp.dot(act_ctx, w_scale, preferred_element_type=jnp.float32)[0]
    pre_query, pre_key, pre_value, onward_leading_sums, reverse_leading_sums = project(latent, norm_gain, shift_lat, scale_lat, (w_query, w_key, w_value, w_decay_fwd, w_decay_bwd))
    cpre_key, cpre_value, conditioning_onward_leading, conditioning_reverse_leading = project(context, norm_gain, shift_ctx, scale_ctx, (w_key, w_value, w_decay_fwd, w_decay_bwd))
    query_rows = divide_among_attention_units(rounded(pre_query), ADDRESS_WIDTH) * ADDRESS_WIDTH ** (-0.5)
    key_lat = divide_among_attention_units(rounded(pre_key), ADDRESS_WIDTH)
    value_lat = divide_among_attention_units(rounded(pre_value), VALUE_DIM)
    context_key_rows = divide_among_attention_units(rounded(cpre_key), ADDRESS_WIDTH)
    context_value_rows = divide_among_attention_units(rounded(cpre_value), VALUE_DIM)
    summand_list = jnp.transpose(decay_log)[:, :, None]
    onward_logarithms = divide_among_attention_units(jax.nn.log_sigmoid(onward_leading_sums + forgetting_shift_vector[None, :]) / smoothing_scale_factor, ADDRESS_WIDTH) + summand_list
    reverse_logarithms = divide_among_attention_units(jax.nn.log_sigmoid(reverse_leading_sums + forgetting_shift_vector[None, :]) / smoothing_scale_factor, ADDRESS_WIDTH) + summand_list
    conditioning_onward_logarithms = divide_among_attention_units(jax.nn.log_sigmoid(conditioning_onward_leading + forgetting_shift_vector[None, :]) / smoothing_scale_factor, ADDRESS_WIDTH)
    conditioning_reverse_logarithms = divide_among_attention_units(jax.nn.log_sigmoid(conditioning_reverse_leading + forgetting_shift_vector[None, :]) / smoothing_scale_factor, ADDRESS_WIDTH)
    cumulative_forward = jnp.cumsum(conditioning_onward_logarithms, axis=1)
    context_forward = jnp.einsum('xcq,xcs->xqs', context_key_rows * jnp.exp(cumulative_forward[:, -1:, :] - cumulative_forward), context_value_rows, precision=highest_precision)
    cumulative_backward = jnp.cumsum(conditioning_reverse_logarithms, axis=1)
    context_backward = jnp.einsum('xcq,xcs->xqs', context_key_rows * jnp.exp(cumulative_backward - conditioning_reverse_logarithms), context_value_rows, precision=highest_precision)
    fwd_out, unused_fwd = blockwise(query_rows, key_lat, value_lat, onward_logarithms, context_forward)
    bwd_flip, unused_bwd = blockwise(jnp.flip(query_rows, 1), jnp.flip(key_lat, 1), jnp.flip(value_lat, 1), jnp.flip(reverse_logarithms, 1), context_backward)
    mixed = fwd_out + jnp.flip(bwd_flip, 1)
    normed = mixed * lax.rsqrt(lax.optimization_barrier(jnp.mean(mixed * mixed, axis=2, keepdims=True)) + epsilon)
    normed = normed * head_gain.reshape(HEADS, 1, VALUE_DIM)
    heads_out = jnp.transpose(normed, (1, 0, 2)).reshape(SEQ, HEADS * VALUE_DIM).astype(jnp.bfloat16)
    projected = contract(heads_out, w_out)
    return (gate_lat[None, :] * projected).astype(jnp.bfloat16)
```

```python
import functools
import heapq
from types import SimpleNamespace

import jax
import jax.numpy as jnp
from jax import lax
from jax.experimental import pallas as pl
from jax.experimental.pallas import tpu as pltpu
from jax.sharding import PartitionSpec as P

f32 = jnp.float32
bf16 = jnp.bfloat16
EPS = 1e-06
STREAMS = (("y", 48, 80), ("x", 0, 48))
FEATS = 128


def halves(n, swap):
    small = (n // 2) // 16 * 16
    return (n - small, small) if swap else (small, n - small)


def gather_plan(X, Y, streams, rate, latency=2.0):
    sizes = {"x": X, "y": Y}
    messages = {}

    def ring(part, axis, base, r0, rows, needs):
        n = sizes[axis]
        swap = (sum(base) % 2) == 1
        for sign in (1, -1):
            for hop in range(1, n // 2 + 1):
                a, b = r0, rows
                if 2 * hop == n:
                    first, second = halves(rows, swap)
                    a, b = (r0, first) if sign == 1 else (r0 + first, second)
                offset = list(base)
                offset[0 if axis == "x" else 1] = sign * hop
                before = [(part, axis, base, sign, hop - 1)] if hop > 1 else list(needs)
                messages[(part, axis, base, sign, hop)] = dict(
                    axis=axis, sign=sign, hop=hop, offset=tuple(offset), a=a, n=b, before=before,
                    left=n // 2 - hop + (10 if part[0] == 1 else 0),
                )

    def origins(axis):
        n = sizes[axis]
        return [h for h in range(-(n // 2) + 1, n // 2 + 1)]

    def arrivals(part, axis, base, value):
        n = sizes[axis]
        if value == 0:
            return []
        if 2 * value == n:
            return [(part, axis, base, s, n // 2) for s in (1, -1)]
        return [(part, axis, base, 1 if value > 0 else -1, abs(value))]

    zero = (0, 0)
    for i, (axis, r0, rows) in enumerate(streams):
        ring((1, i), axis, zero, r0, rows, [])
        for v in origins(axis):
            base = (v, 0) if axis == "x" else (0, v)
            ring((2, i), "y" if axis == "x" else "x", base, r0, rows, arrivals((1, i), axis, zero, v))

    return simulate(messages, 768, rate, latency)


def simulate(messages, row_bytes, rate, latency):
    keys = list(messages)
    index = {k: i for i, k in enumerate(keys)}
    free = {(a, s): 0.0 for a in ("x", "y", "all") for s in (1, -1)}
    got, order, started, heap = set(), [], set(), []

    def launch(now):
        ready = [k for k in keys if k not in started and all(b in got for b in messages[k]["before"])]
        ready.sort(key=lambda k: -messages[k]["left"])
        for k in ready:
            m = messages[k]
            link = (m["axis"], m["sign"])
            begin = max(now, free[link])
            hops = m.get("step", 1)
            free[link] = begin + hops * m["n"] * row_bytes / rate
            heapq.heappush(heap, (free[link] + latency + 0.8 * (hops - 1), index[k]))
            started.add(k)
        return [index[k] for k in ready]

    first = launch(0.0)
    steps = []
    while heap:
        now, i = heapq.heappop(heap)
        got.add(keys[i])
        steps.append((i, launch(now), now))
    table = [messages[k] for k in keys]
    return table, first, steps


def share_plan(X, Y, rows, rate, latency=2.0):
    messages = {}
    half = Y // 2
    for v in range(-(X // 2) + 1, X // 2 + 1):
        if v:
            messages[("all", v)] = dict(axis="all", sign=1 if v > 0 else -1, offset=(v, 0), a=0, n=rows, before=[], left=20)
        for sign in (1, -1):
            for hop in range(1, half + 1):
                a, b = 0, rows
                if 2 * hop == Y:
                    first, second = halves(rows, v % 2 == 1)
                    a, b = (0, first) if sign == 1 else (first, second)
                step = 2 if hop % 2 == 0 else 1
                before = [(v, sign, hop - step)] if hop > 2 else [("all", v)] if v else []
                messages[(v, sign, hop)] = dict(
                    axis="y", sign=sign, offset=(v, sign * hop), a=a, n=b, before=before, step=step,
                    left=10 * (half - hop >= 2 and step == 2) + step,
                )
    return simulate(messages, 256, rate, latency)


def rows_done(plan, X, Y):
    table, _, steps = plan
    left = {}
    for m in table:
        oy = m["offset"][1] % Y
        left[oy] = left.get(oy, 0) + 1
    out = []
    for i, _, _ in steps:
        oy = table[i]["offset"][1] % Y
        left[oy] -= 1
        out.append([oy] if left[oy] == 0 else [])
    return out


def split3(v):
    hi = v.astype(bf16)
    r = v - hi.astype(f32)
    mid = r.astype(bf16)
    return hi, mid, (r - mid.astype(f32)).astype(bf16)


def mm(a, b):
    return lax.dot_general(a, b, (((1,), (0,)), ((), ())), preferred_element_type=f32)


def nt(a, b):
    return lax.dot_general(a, b, (((1,), (1,)), ((), ())), preferred_element_type=f32)


def iota(shape, dim):
    return lax.broadcasted_iota(jnp.int32, shape, dim)


def kernel(dims, *refs):
    X, Y, Z, HALF, WIDTH = dims
    NC = X * Y
    TILES = HALF // 128
    NB = 2 * TILES
    GK = X * FEATS
    names = (
        "lat", "ctx", "cond", "cctx", "ws", "wc", "wg", "gain",
        "wq", "wk", "wv", "wf", "wb", "fsv", "dl", "hg",
        "wo", "out", "xg", "xs", "wall", "wog", "gcol", "acc",
        "acc2", "hrow", "hq", "res", "obuf", "ctxo", "ctxp", "ctxm", "ctxg",
        "vec", "fsb", "vecp", "wm", "cnd", "zblk", "zred", "mblk",
        "mrecv", "xyblk", "xyg", "dlv", "pst", "tst",
        "qst", "ost", "zs1", "zs1r", "zmsg", "zrcv", "zent", "ent",
        "cs1", "cs1r", "cmsg", "crcv", "crcv2", "cpk", "loc_sem", "dd_send", "dd_recv",
        "ag1_send", "ag1_recv", "ag2_send", "ag2_recv", "z_send", "z_recv", "xy_send", "xy_recv",
        "cx_send", "cx_recv", "zc_send", "zc_recv", "zl_send", "zl_recv", "wg_send", "wg_recv", "o_send", "o_recv",
    )
    r = SimpleNamespace(**dict(zip(names, refs, strict=True)))

    z = lax.axis_index("sp")
    tp = lax.axis_index("tp")
    c = lax.rem(tp, 2)
    chip = lax.div(tp, 2)
    x = lax.rem(chip, X)
    y = lax.div(chip, X)
    o = 1 - c

    def along_x(step):
        return at(z, lax.rem(x + step + X, X), y, c)

    scopes = []

    def mark(name):
        if scopes:
            scopes.pop().__exit__(None, None, None)
        if name:
            s = jax.named_scope(name)
            s.__enter__()
            scopes.append(s)

    mark("start")

    def at(zz, xx, yy, cc):
        return (zz, (yy * X + xx) * 2 + cc)

    partner = at(z, x, y, o)
    far = lambda d, n: min(d, n - d)
    zstep = sorted(range(1, Z), key=lambda j: -far(j, Z))
    zpeer = [at(lax.rem(z + j, Z), x, y, c) for j in zstep]
    offs = [(dx, dy) for dy in range(Y) for dx in range(X) if dx or dy]
    offs.sort(key=lambda d: -far(d[0], X) - far(d[1], Y))
    xypeer = [at(z, lax.rem(x + dx, X), lax.rem(y + dy, Y), c) for dx, dy in offs]

    def remote(src, dst, ssem, rsem, dev):
        return pltpu.make_async_remote_copy(
            src_ref=src, dst_ref=dst, send_sem=ssem, recv_sem=rsem,
            device_id=dev, device_id_type=pl.DeviceIdType.MESH,
        )

    def wait_sends(ref, ssem, rsem):
        remote(ref, ref, ssem, rsem, partner).wait_send()

    def wait_recvs(ref, ssem, rsem):
        remote(ref, ref, ssem, rsem, partner).wait_recv()

    half = pl.ds(pl.multiple_of(c * HALF, 128), HALF)
    other = pl.ds(pl.multiple_of(o * HALF, 128), HALF)
    wrows = (("wq", 0, 32), ("wk", 64, 32), ("wv", 128, 64), ("wf", 256, 32), ("wb", 320, 32))

    def mine(base, n):
        return pl.ds(pl.multiple_of(base + c * n, 16), n)

    local = []

    def bring(src, dst):
        cp = pltpu.make_async_copy(src, dst, r.loc_sem.at[len(local)])
        cp.start()
        local.append(cp)

    bring(r.cond, r.cnd.at[0])
    bring(r.cctx, r.cnd.at[1])
    bring(r.ws, r.wm.at[0])
    bring(r.wc, r.wm.at[1])
    bring(r.wg, r.wm.at[2])
    bring(r.gain, r.vec.at[0])
    bring(r.hg, r.vec.at[1])
    bring(r.fsv, r.fsb)
    n_first = len(local)
    bring(r.ctx.at[pl.ds(pl.multiple_of(c * 16, 16), 16)], r.ctxo)
    bring(r.lat.at[:, half], r.xg.at[chip, mine(0, 64)])
    n_second = len(local)
    bring(r.dl.at[:, half], r.dlv.at[0])
    for name, base, n in wrows:
        bring(getattr(r, name), r.wall.at[mine(base, n)])
    bring(r.wo, r.wog.at[x, mine(0, 64)])

    barrier = pltpu.get_barrier_semaphore()
    peers = [partner] + xypeer + zpeer
    for dev in peers:
        pl.semaphore_signal(barrier, inc=1, device_id=dev, device_id_type=pl.DeviceIdType.MESH)
    for cp in local[:n_first]:
        cp.wait()

    kw = r.cnd.shape[2]
    row8 = iota((8, kw), 0)
    cl = r.cnd[0]
    cc = r.cnd[1]
    al = (cl * jax.nn.sigmoid(cl)).astype(bf16).astype(f32)
    ac = (cc * jax.nn.sigmoid(cc)).astype(bf16).astype(f32)
    act = jnp.where(row8 == 1, jnp.broadcast_to(ac, (8, kw)), jnp.broadcast_to(al, (8, kw))).astype(bf16)
    d1 = nt(act, jnp.concatenate([r.wm[0], r.wm[1]], axis=0))
    d2 = nt(act, jnp.concatenate([r.wm[2], r.wm[2]], axis=0))
    r8 = iota((8, 128), 0)
    l8 = iota((8, 128), 1)
    part = jnp.where(r8 < 2, d1, d2)
    r.zblk[...] = part
    hg64 = r.vec[1]
    gn64 = r.vec[0]
    hgd = jnp.concatenate([hg64, hg64], axis=1)
    gnd = jnp.concatenate([gn64, gn64], axis=1)
    f1 = r.fsb[...]
    fsd = jnp.concatenate([f1, f1, f1, f1], axis=1)
    vown = jnp.where(r8 == 0, hgd, jnp.where(r8 == 1, fsd, gnd))
    r.mblk[pl.ds(16, 8)] = vown

    mark("barrier")
    pl.semaphore_wait(barrier, len(peers))

    mark("sends")
    for j, dev in enumerate(zpeer):
        cp = remote(r.zblk.at[pl.ds(0, 4)], r.zred.at[z, pl.ds(0, 4)], r.z_send, r.z_recv, dev)
        cp.start()
    dd = []

    def give(src, dst):
        k = len(dd)
        cp = remote(src, dst, r.dd_send.at[k], r.dd_recv.at[k], partner)
        cp.start()
        dd.append(cp)
        return cp

    d_lat = give(r.lat.at[:, other], r.xg.at[chip, mine(0, 64)])
    d_ctx = give(r.ctx.at[pl.ds(pl.multiple_of(o * 16, 16), 16)], r.ctxp)
    for cp in local[n_first:n_second]:
        cp.wait()

    plan = gather_plan(X, Y, STREAMS, 42.0e3, 2.8)
    table = plan[0]

    def gather(plan, buf, ssem, rsem, after):
        table, first, steps = plan
        copies = {}

        def slot_of(ox, oy):
            return lax.rem(y - oy + Y, Y) * X + lax.rem(x - ox + X, X)

        def go(i):
            m = table[i]
            ox, oy = m["offset"]
            if m["axis"] == "all":
                to = lax.rem(x + ox + X, X)
                src = r.hrow.at[pl.ds(pl.multiple_of(to * m["n"], 16), m["n"])]
                dst, dev = buf.at[chip], along_x(ox)
            else:
                if m["axis"] == "x":
                    dev = along_x(m["sign"])
                    slot = slot_of(ox - m["sign"], oy)
                else:
                    step = m["sign"] * m.get("step", 1)
                    dev = at(z, x, lax.rem(y + step + Y, Y), c)
                    slot = slot_of(ox, oy - step)
                src = dst = buf.at[slot, pl.ds(m["a"], m["n"])]
            copies[i] = remote(src, dst, ssem, rsem.at[i], dev)
            copies[i].start()

        for i in first:
            go(i)
        after(-1, 0.0)
        for s, (i, then, when) in enumerate(steps):
            m = table[i]
            ref = buf.at[slot_of(*m["offset"]), pl.ds(m["a"], m["n"])]
            wait_recvs(ref, ssem, rsem.at[i])
            for k in then:
                go(k)
            after(s, when)
        return copies

    lane128 = l8[:1]
    mylane = lane128 // 64 == c

    def join(own, recv, lanes):
        return jnp.where(lanes // 64 == c, own, recv)

    state = {}

    def send_ctx():
        d_ctx.wait_recv()
        own = r.ctxo[...].astype(f32)
        rec = r.ctxp[...].astype(f32)
        lo = jnp.where(c == 0, own, rec)
        hi = jnp.where(c == 0, rec, own)
        both = jnp.concatenate([lo, hi], axis=1).astype(bf16)
        r.ctxm[...] = both
        r.ctxg[chip] = both
        for j, dev in enumerate(xypeer):
            cp = remote(r.ctxm, r.ctxg.at[chip], r.cx_send, r.cx_recv, dev)
            cp.start()

    def send_weights():
        state["wd1"] = [give(getattr(r, name), r.wall.at[mine(base, n)]) for name, base, n in wrows]
        state["wd1"].append(give(r.dl.at[:, other], r.dlv.at[1]))
        state["wd1"].append(give(r.wo, r.wog.at[x, mine(0, 64)]))

    def z_sum():
        wait_recvs(r.zred.at[pl.ds(0, Z - 1), pl.ds(0, 4)], r.z_send, r.z_recv)
        r.zred[z] = part
        M = r.zred[0][0:4]
        for j in range(1, Z):
            M = M + r.zred[j][0:4]
        M = jnp.concatenate([M, M], axis=0)
        rM = pltpu.roll(M, 64, 1)
        r.mblk[pl.ds(0, 8)] = jnp.where(l8 < 64, M, rM)
        r.mblk[pl.ds(8, 8)] = jnp.where(l8 < 64, rM, M)
        state["mod"] = give(r.mblk, r.mrecv)

    def xy_send():
        state["mod"].wait_recv()
        lanes = iota((24, 128), 1)
        rws = iota((24, 128), 0)
        pick = jnp.where(rws == 17, (lanes // 32) % 2, lanes // 64)
        both = jnp.where(pick == c, r.mblk[...], r.mrecv[...])
        A = both[0:8]
        B = both[8:16]
        V = both[16:24]
        r.vecp[...] = jnp.where(r8 < 2, V, jnp.where(r8 == 2, A, 0.0))
        G = V[2:3] * (1.0 + B)
        blk = jnp.where(r8 < 2, A, jnp.where(r8 < 4, pltpu.roll(G, 2, 0), pltpu.roll(A, 2, 0)))
        r.xyblk[...] = blk
        r.xyg[chip] = blk
        for j, dev in enumerate(xypeer):
            cp = remote(r.xyblk, r.xyg.at[chip], r.xy_send, r.xy_recv, dev)
            cp.start()

    def w_part(slot, a, n):
        return r.wog.at[lax.rem(slot + X, X), pl.ds(pl.multiple_of(c * 64 + a, 16), n)]

    wg = []

    def w_ring(sign, slot, a, n):
        k = len(wg)
        ref = w_part(slot, a, n)
        cp = remote(ref, ref, r.wg_send.at[k], r.wg_recv.at[k], along_x(sign))
        cp.start()
        wg.append((cp, slot - sign, a, n))

    def w_landed(k):
        _, slot, a, n = wg[k]
        ref = w_part(slot, a, n)
        remote(ref, ref, r.wg_send.at[k], r.wg_recv.at[k], partner).wait_recv()
        return give(ref, ref)

    def w_first():
        if X == 2:
            w_ring(1, x, 0, 32)
            w_ring(-1, x, 32, 32)
        else:
            w_ring(1, x, 0, 64)
            w_ring(-1, x, 0, 64)

    def w_second():
        state["wd"] = [w_landed(0), w_landed(1)]
        if X == 4:
            w_ring(1, x - 1, 0, 32)
            w_ring(-1, x + 1, 32, 32)

    def w_third():
        if X == 4:
            state["wd"] += [w_landed(2), w_landed(3)]
        for cp in state["wd"]:
            cp.wait_recv()

    def cols_of(v):
        return jnp.transpose(jnp.concatenate([v, jnp.zeros((120, 128), f32)], axis=0))

    row128 = iota((128, 128), 0)
    ln128 = iota((128, 128), 1)
    same = (row128 // 64) == (ln128 // 64)
    tri = jnp.where(same & (row128 <= ln128), 1.0, 0.0).astype(bf16)
    blk_ones = jnp.where(same, 1.0, 0.0).astype(bf16)
    sums = jnp.concatenate([tri, blk_ones], axis=1)
    ind = jnp.where((r8 < 2) & (l8 // 64 == r8), 1.0, 0.0).astype(bf16)
    head_lane = (lane128 // 32) % 2
    mf = same & (row128 <= ln128)
    mb = same & (row128 >= ln128)

    def exponents(L):
        hi, mid, lo = split3(L)
        big = mm(jnp.concatenate([hi, mid, lo], axis=0), sums)
        big = big[0:128] + big[128:256] + big[256:384]
        C, T = big[:, 0:128], big[:, 128:256]
        E = jnp.where(row128 < 64, C, T - C + L)
        tot = nt(ind, hi) + nt(ind, mid) + nt(ind, lo)
        return E, T - E, tot

    def terms(k2, vT, D):
        ks = k2 * jnp.exp(D)
        stack = jnp.concatenate(
            [jnp.where(ln128 < 64, ks, 0.0).astype(bf16), jnp.where(ln128 < 64, 0.0, ks).astype(bf16)], axis=0
        )
        K = nt(vT, stack)
        first = jnp.where(head_lane == 0, K[0:64, 0:128], K[64:128, 0:128])
        second = jnp.where(head_lane == 0, K[0:64, 128:256], K[64:128, 128:256])
        return first, second

    def log_sigmoid(v):
        return jnp.minimum(v, 0.0) - jnp.log1p(jnp.exp(-jnp.abs(v)))

    lane64 = iota((64, 128), 1)
    lane32 = iota((32, 128), 1)
    lane16 = iota((16, 128), 1)

    def chip_state(stage, recv, own_ref):
        own = own_ref[pl.ds(pl.multiple_of(c * 32, 8), 32)]
        rec = recv[pl.ds(0, 32)]
        town = stage[pl.ds(32, 1)]
        trec = recv[pl.ds(32, 1)]
        s0 = jnp.where(c == 0, own, rec)
        s1 = jnp.where(c == 0, rec, own)
        t0 = jnp.where(c == 0, town, trec)
        t1 = jnp.where(c == 0, trec, town)
        both = jnp.where(lane32 < 64, jnp.exp(t1) * s0 + s1, jnp.exp(t0) * s1 + s0)
        return both, t0, t1, s0, s1

    def log_rows(T):
        hi = T.astype(bf16).astype(f32)
        return jnp.where(iota((16, 128), 0) == 0, hi, jnp.where(iota((16, 128), 0) == 1, T - hi, 0.0))

    def mod_in():
        wait_recvs(r.xyg.at[pl.ds(0, NC - 1)], r.xy_send, r.xy_recv)
        wait_recvs(r.ctxg.at[pl.ds(0, NC - 1)], r.cx_send, r.cx_recv)
        for cp in local[n_second:]:
            cp.wait()
        for cp in state["wd1"]:
            cp.wait_recv()

        for q in range(max(NC // 16, 1)):
            n = min(NC, 16)
            rows = r.xyg[pl.ds(q * n, n)].reshape(n * 8, 128)
            if n < 16:
                rows = jnp.concatenate([rows, jnp.zeros((128 - n * 8, 128), f32)], axis=0)
            t = jnp.transpose(rows)
            for b in range(n):
                r.gcol[q * n + b] = jnp.broadcast_to(t[:, b * 8 + 2 : b * 8 + 3], (128, 128))

    def ctx_work(sq):
        pcv = r.acc[:, pl.ds(HALF, 128)]
        sqt = jnp.transpose(jnp.concatenate([sq, jnp.zeros((112, 128), f32)], axis=0))
        ssum = jnp.sum(sqt, axis=0, keepdims=True)
        inv = lax.rsqrt(ssum / WIDTH + EPS)
        cp_ = inv * pcv + pcv[:, 17:18]
        valid = ln128 < 16
        k = jnp.where(valid[0:64], cp_[64:128], 0.0).astype(bf16).astype(f32)
        k2 = jnp.concatenate([k, k], axis=0)
        vT = jnp.where(valid, cp_[128:256], 0.0).astype(bf16)
        colv = cols_of(r.vecp[...])
        L = jnp.where(valid, log_sigmoid(cp_[256:384] + colv[:, 1:2]) / 16.0, 0.0)
        E, D, tot = exponents(L)
        first, _ = terms(k2, vT, D)
        r.cpk[...] = first
        r.cs1[pl.ds(0, 32)] = jnp.where(c == 0, first[32:64], first[0:32])
        r.cs1[pl.ds(32, 8)] = jnp.broadcast_to(tot[0:1], (8, 128))
        state["c1"] = give(r.cs1, r.cs1r)

    G = min(4, Z)
    za, zb = lax.div(z, G), lax.rem(z, G)

    def ctx_message(both, T):
        return jnp.concatenate([both, log_rows(T)[0:8]], axis=0).astype(bf16)

    def ctx_fold(ref, n):
        sf = sb = T = None
        for i in range(n):
            m = ref[i].astype(f32)
            t = m[32:33] + m[33:34]
            sf = m[0:32] if i == 0 else jnp.exp(t) * sf + m[0:32]
            T = t if i == 0 else T + t
            m = ref[n - 1 - i].astype(f32)
            sb = m[0:32] if i == 0 else jnp.exp(m[32:33] + m[33:34]) * sb + m[0:32]
        return jnp.where(lane32 < 64, sf, sb), T

    def ctx_send():
        state["c1"].wait_recv()
        both, t0, t1, _, _ = chip_state(r.cs1, r.cs1r, r.cpk)
        msg = ctx_message(both, t0 + t1)
        r.cmsg[0] = msg
        r.crcv[zb] = msg
        for j in range(1, G):
            dev = at(za * G + lax.rem(zb + j, G), x, y, c)
            cp = remote(r.cmsg.at[0], r.crcv.at[zb], r.zc_send.at[0], r.zc_recv.at[0], dev)
            cp.start()

    def ctx_second():
        wait_recvs(r.crcv.at[pl.ds(0, G - 1)], r.zc_send.at[0], r.zc_recv.at[0])
        both, T = ctx_fold(r.crcv, G)
        msg = ctx_message(both, T)
        r.cmsg[1] = msg
        r.crcv2[za] = msg
        for j in range(1, Z // G):
            dev = at(lax.rem(z + j * G, Z), x, y, c)
            cp = remote(r.cmsg.at[1], r.crcv2.at[za], r.zc_send.at[1], r.zc_recv.at[1], dev)
            cp.start()

    def ctx_done():
        if Z > G:
            wait_recvs(r.crcv2.at[pl.ds(0, Z // G - 1)], r.zc_send.at[1], r.zc_recv.at[1])
        r.cpk[pl.ds(0, 32)] = ctx_fold(r.crcv2, Z // G)[0]

    sums_of = {"lat": [jnp.zeros((8, 128), f32) for _ in range(TILES)], "ctx": jnp.zeros((16, 128), f32), "n": 0}

    def project(yy):
        for xx in range(X):
            b = yy * X + xx
            xr = pl.ds(xx * 128, 128)
            for t in range(TILES):
                v = r.xg[b, :, pl.ds(t * 128, 128)].astype(f32)
                s2 = v * v
                part_s = s2[0:8]
                for q in range(1, 16):
                    part_s = part_s + s2[q * 8 : q * 8 + 8]
                sums_of["lat"][t] = sums_of["lat"][t] + part_s
                r.xs[xr, pl.ds(t * 128, 128)] = (v * r.gcol[b]).astype(bf16)
            m = r.xyg[b]
            raw = r.ctxg[b].astype(f32)
            sums_of["ctx"] = sums_of["ctx"] + raw * raw
            rows = jnp.concatenate([raw * m[3:4], m, jnp.zeros((104, 128), f32)], axis=0)
            r.xs[xr, pl.ds(HALF, 128)] = jnp.transpose(rows).astype(bf16)
        step = mm(r.wall[:, pl.ds(pl.multiple_of(yy * GK, 128), GK)], r.xs[...])
        r.acc[...] = step if sums_of["n"] == 0 else r.acc[...] + step
        sums_of["n"] += 1

    actions = [(9.5, z_sum), (10.3, xy_send), (10.8, send_ctx), (12.0, send_weights)]
    pending = list(actions)
    rows1 = rows_done(plan, X, Y)
    last_go = max(i for i, st in enumerate(plan[2]) if st[1])
    waiting = []

    def after1(s, when):
        if s < 0:
            return
        while pending and pending[0][0] <= when:
            fn = pending.pop(0)[1]
            with jax.named_scope(fn.__name__):
                fn()
        waiting.extend(rows1[s])
        if s == last_go:
            while pending:
                pending.pop(0)[1]()
            with jax.named_scope("mod_in"):
                mod_in()
            w_first()
        if s >= last_go:
            while waiting:
                with jax.named_scope("project"):
                    project(lax.rem(y - waiting.pop(0) + Y, Y))

    mark("d_lat")
    d_lat.wait_recv()
    mark("ag1")
    copies1 = gather(plan, r.xg, r.ag1_send, r.ag1_recv, after1)
    ss = sums_of["lat"]

    mark("attend")
    colv = cols_of(r.vecp[...])
    shift_col = r.acc[:, pl.ds(HALF, 128)][:, 16:17]
    own_dl = r.dlv[0]
    rec_dl = r.dlv[1]
    dl0 = jnp.where(c == 0, own_dl, rec_dl)
    dl1 = jnp.where(c == 0, rec_dl, own_dl)
    for t in range(TILES):
        ts = pl.ds(t * 128, 128)
        inv = lax.rsqrt(jnp.sum(ss[t], axis=0, keepdims=True) / WIDTH + EPS)
        pr = inv * r.acc[:, ts] + shift_col
        q = pr[0:64].astype(bf16).astype(f32) * (32.0 ** -0.5)
        k = pr[64:128].astype(bf16).astype(f32)
        vT = pr[128:256].astype(bf16)
        q2 = jnp.concatenate([q, q], axis=0)
        k2 = jnp.concatenate([k, k], axis=0)
        dlt = jnp.where((row128 // 32) % 2 == 0, dl0[:, t * 128 : t * 128 + 128], dl1[:, t * 128 : t * 128 + 128])
        L = log_sigmoid(pr[256:384] + colv[:, 1:2]) / 16.0 + dlt
        E, D, tot = exponents(L)
        first, second = terms(k2, vT, D)
        r.pst[2 * t] = first
        r.pst[2 * t + 1] = second
        r.tst[t] = tot
        qf = q2 * jnp.exp(E)
        r.qst[t] = qf
        r.ost[t, 0] = k2 * jnp.exp(-E)
        r.ost[t, 1] = vT.astype(f32)

    T = [r.tst[i // 2][i % 2 : i % 2 + 1] for i in range(NB)]
    e = [jnp.exp(v) for v in T]
    sf = jnp.zeros((64, 128), f32)
    sb = jnp.zeros((64, 128), f32)
    for i in range(NB):
        sf = e[i] * sf + r.pst[i]
        sb = e[NB - 1 - i] * sb + r.pst[NB - 1 - i]
    seg = jnp.where(lane64 < 64, sf, sb)
    tseg = sum(T[1:], T[0])
    r.zent[...] = seg
    r.zs1[pl.ds(0, 32)] = jnp.where(c == 0, seg[32:64], seg[0:32])
    r.zs1[pl.ds(32, 8)] = jnp.broadcast_to(tseg, (8, 128))
    d_seg = give(r.zs1, r.zs1r)
    mark("ctx_work")
    ctx_work(sums_of["ctx"])
    mark("d_seg")
    ctx_send()
    d_seg.wait_recv()
    mark("combine")
    both, t0, t1, s0, s1 = chip_state(r.zs1, r.zs1r, r.zent)
    tc = t0 + t1
    rtc = pltpu.roll(jnp.broadcast_to(tc, (8, 128)), 64, 1)[0:1]
    ra = pltpu.roll(both[0:16], 64, 1)
    rb = pltpu.roll(both[16:32], 64, 1)
    r.zmsg[0] = jnp.concatenate(
        [jnp.where(lane16 < 64, both[0:16], rb), log_rows(jnp.where(lane128 < 64, tc, rtc))[0:8]], axis=0
    ).astype(bf16)
    r.zmsg[1] = jnp.concatenate(
        [jnp.where(lane16 < 64, ra, both[16:32]), log_rows(jnp.where(lane128 < 64, rtc, tc))[0:8]], axis=0
    ).astype(bf16)
    r.zrcv[z] = jnp.zeros((24, 128), bf16)
    for j, dev in enumerate(zpeer):
        behind = jnp.where(z + zstep[j] >= Z, 1, 0)
        cp = remote(r.zmsg.at[behind], r.zrcv.at[z], r.zl_send, r.zl_recv, dev)
        cp.start()

    mark("scores")
    for t in range(TILES):
        qf = r.qst[t]
        kdT = jnp.transpose(r.ost[t, 0]).astype(bf16)
        vT = r.ost[t, 1].astype(bf16)
        parts = [jnp.where(row128 // 32 == i, qf, 0.0).astype(bf16) for i in range(4)]
        AT = mm(kdT, jnp.concatenate(parts, axis=1))
        A0 = jnp.where(mf, AT[:, 0:128], 0.0) + jnp.where(mb, AT[:, 256:384], 0.0)
        A1 = jnp.where(mf, AT[:, 128:256], 0.0) + jnp.where(mb, AT[:, 384:512], 0.0)
        r.ost[t, 1] = jnp.concatenate(
            [mm(vT[0:64], A0.astype(bf16)), mm(vT[64:128], A1.astype(bf16))], axis=0
        )

    mark("ctx_second")
    ctx_second()
    mark("ctx_done")
    ctx_done()
    mark("zwait")
    wait_recvs(r.zrcv.at[pl.ds(0, Z - 1)], r.zl_send, r.zl_recv)
    mark("entering")
    ctxs = r.cpk[pl.ds(0, 32)]
    ca = pltpu.roll(ctxs[0:16], 64, 1)
    cb = pltpu.roll(ctxs[16:32], 64, 1)
    ef = jnp.where(lane16 < 64, ctxs[0:16], cb)
    eb = jnp.where(lane16 < 64, ca, ctxs[16:32])
    for s in range(Z):
        m = r.zrcv[s].astype(f32)
        ef = jnp.where(s < z, jnp.exp(m[16:17] + m[17:18]) * ef + m[0:16], ef)
        u = Z - 1 - s
        m = r.zrcv[u].astype(f32)
        eb = jnp.where(u > z, jnp.exp(m[16:17] + m[17:18]) * eb + m[0:16], eb)
    ech = jnp.concatenate(
        [
            jnp.where(lane16 < 64, ef, pltpu.roll(eb, 64, 1)),
            jnp.where(lane16 < 64, pltpu.roll(ef, 64, 1), eb),
        ],
        axis=0,
    )
    ent0 = jnp.where(lane32 < 64, ech, jnp.exp(t1) * ech + s1)
    ent1 = jnp.where(lane32 < 64, jnp.exp(t0) * ech + s0, ech)
    rows_c = pl.ds(pl.multiple_of(c * 32, 8), 32)
    d_seg.wait_send()
    r.zs1[pl.ds(0, 32)] = jnp.where(c == 0, ent1, ent0)
    r.ent[rows_c] = jnp.where(c == 0, ent0, ent1)
    mark("d_ent")
    d_ent = give(r.zs1.at[pl.ds(0, 32)], r.ent.at[rows_c])
    d_ent.wait_recv()

    mark("post")
    sf = r.ent[...]
    sb = sf
    fin, bin_ = [None] * NB, [None] * NB
    for i in range(NB):
        fin[i] = sf
        sf = e[i] * sf + r.pst[i]
        u = NB - 1 - i
        bin_[u] = sb
        sb = e[u] * sb + r.pst[u]
    hcol = colv[:, 0:1]
    for t in range(TILES):
        qf = r.qst[t]
        lhs = []
        for i in (2 * t, 2 * t + 1):
            s_in = jnp.where(lane64 < 64, fin[i], bin_[i])
            lhs.append(
                jnp.concatenate(
                    [jnp.where(head_lane == 0, s_in, 0.0), jnp.where(head_lane == 1, s_in, 0.0)], axis=0
                ).astype(bf16)
            )
        rhs = jnp.concatenate(
            [jnp.where(ln128 < 64, qf, 0.0).astype(bf16), jnp.where(ln128 < 64, 0.0, qf).astype(bf16)], axis=0
        )
        mixed = r.ost[t, 1] + mm(jnp.concatenate(lhs, axis=1), rhs)
        outs = []
        for h in range(2):
            mh = mixed[h * 64 : h * 64 + 64]
            outs.append(mh * lax.rsqrt(jnp.mean(mh * mh, axis=0, keepdims=True) + EPS))
        heads = jnp.concatenate(outs, axis=0) * hcol
        r.hrow[pl.ds(t * 128, 128)] = jnp.transpose(heads).astype(bf16)

    mark("ag2")
    TQ = HALF // X
    plan2 = share_plan(X, Y, TQ, 46.0e3, 2.8)
    r.hq[chip] = r.hrow[pl.ds(pl.multiple_of(x * TQ, 16), TQ)]
    done2 = rows_done(plan2, X, Y)
    ready2 = []

    def product(yy):
        heads = jnp.concatenate([r.hq[yy * X + xx] for xx in range(X)], axis=1)
        ks = pl.ds(pl.multiple_of(yy * GK, 128), GK)
        step = nt(r.wog[:, :, ks].reshape(X * 128, GK), heads)
        r.acc2[...] = step if not ready2 else r.acc2[...] + step
        ready2.append(yy)

    last_go2 = max([i for i, st in enumerate(plan2[2]) if st[1]], default=-1)
    waiting2 = []

    def after2(s, when):
        if s < 0:
            w_second()
            return
        waiting2.extend(done2[s])
        if s == len(plan2[2]) - 1:
            with jax.named_scope("w_third"):
                w_third()
            while waiting2:
                product(lax.rem(y - waiting2.pop(0) + Y, Y))

    copies2 = gather(plan2, r.hq, r.ag2_send, r.ag2_recv, after2)
    mark("final")
    gates = jnp.concatenate([r.xyg[y * X + xx][4:5] for xx in range(X)] + [jnp.zeros((8 - X, 128), f32)], axis=0)
    gates = cols_of(gates)
    for xx in range(X):
        piece = (r.acc2[pl.ds(xx * 128, 128)] * gates[:, xx : xx + 1]).astype(bf16)
        r.res[xx, 0] = piece[0:64]
        r.res[xx, 1] = piece[64:128]
    mine_at = 2 * x + c
    for dx, dc in [(dx, dc) for dx in (2, 1, 3, 0) if dx < X for dc in (0, 1) if dx or dc]:
        tx = lax.rem(x + dx, X)
        tc_ = lax.rem(c + dc, 2)
        cp = remote(
            r.res.at[tx, tc_], r.obuf.at[mine_at], r.o_send, r.o_recv, at(z, tx, y, tc_)
        )
        cp.start()
    r.obuf[mine_at] = r.res[x, c]
    wait_recvs(r.obuf.at[pl.ds(0, 2 * X - 1)], r.o_send, r.o_recv)
    r.out[...] = jnp.concatenate([r.obuf[2 * xx + cc_] for cc_ in (0, 1) for xx in range(X)], axis=1)
    mark("drain")
    for cp2 in dd:
        if cp2 is not d_seg:
            cp2.wait_send()
    wait_sends(r.zred.at[pl.ds(0, Z - 1), pl.ds(0, 4)], r.z_send, r.z_recv)
    wait_sends(r.ctxg.at[pl.ds(0, NC - 1)], r.cx_send, r.cx_recv)
    wait_sends(r.xyg.at[pl.ds(0, NC - 1)], r.xy_send, r.xy_recv)
    wait_sends(r.crcv.at[pl.ds(0, G - 1)], r.zc_send.at[0], r.zc_recv.at[0])
    if Z > G:
        wait_sends(r.crcv2.at[pl.ds(0, Z // G - 1)], r.zc_send.at[1], r.zc_recv.at[1])
    wait_sends(r.zrcv.at[pl.ds(0, Z - 1)], r.zl_send, r.zl_recv)
    wait_sends(r.obuf.at[pl.ds(0, 2 * X - 1)], r.o_send, r.o_recv)
    for cp2, _, _, _ in wg:
        cp2.wait_send()
    wait_sends(r.xg.at[pl.ds(0, NC - 1)], r.ag1_send, r.ag1_recv.at[0])
    wait_sends(r.hq.at[pl.ds(0, NC - 1)], r.ag2_send, r.ag2_recv.at[0])
    mark(None)


def per_device(
    latent, context, cond, ctx_cond, w_shift, w_scale, w_gate, norm_gain, w_query, w_key, w_value,
    w_decay_fwd, w_decay_bwd, forgetting_shift_vector, decay_log, head_gain, w_out,
):
    Z = lax.axis_size("sp")
    NC = lax.axis_size("tp") // 2
    X = 4 if NC >= 8 else 2
    Y = NC // X
    tok = latent.shape[0]
    HALF = tok // 2
    WIDTH = w_out.shape[1]
    dims = (X, Y, Z, HALF, WIDTH)
    TILES = HALF // 128
    M = len(gather_plan(X, Y, STREAMS, 46.0e3)[0])
    M2 = len(share_plan(X, Y, HALF // X, 46.0e3)[0])
    V = pltpu.VMEM
    D = pltpu.SemaphoreType.DMA
    GK = X * FEATS
    kw = cond.shape[0]
    scratch = [
        V((NC, 128, HALF), bf16),
        V((GK, HALF + 128), bf16),
        V((384, WIDTH), bf16),
        V((X, 128, WIDTH), bf16),
        V((NC, 128, 128), f32),
        V((384, HALF + 128), f32),
        V((X * 128, HALF // X), f32),
        V((HALF, 128), bf16),
        V((NC, HALF // X, 128), bf16),
        V((X, 2, 64, HALF // X), bf16),
        V((2 * X, 64, HALF // X), bf16),
        V((16, 64), bf16),
        V((16, 64), bf16),
        V((16, 128), bf16),
        V((NC, 16, 128), bf16),
        V((2, 1, 64), f32),
        V((1, 32), f32),
        V((8, 128), f32),
        V((3, 64, kw), bf16),
        V((2, 1, kw), f32),
        V((8, 128), f32),
        V((Z, 8, 128), f32),
        V((24, 128), f32),
        V((24, 128), f32),
        V((8, 128), f32),
        V((NC, 8, 128), f32),
        V((2, 1, HALF), f32),
        V((2 * TILES, 64, 128), f32),
        V((TILES, 8, 128), f32),
        V((TILES, 128, 128), f32),
        V((TILES, 2, 128, 128), f32),
        V((40, 128), f32),
        V((40, 128), f32),
        V((2, 24, 128), bf16),
        V((Z, 24, 128), bf16),
        V((64, 128), f32),
        V((64, 128), f32),
        V((40, 128), f32),
        V((40, 128), f32),
        V((2, 40, 128), bf16),
        V((4, 40, 128), bf16),
        V((4, 40, 128), bf16),
        V((64, 128), f32),
        D((17,)), D((17,)), D((17,)),
        D, D((M,)), D, D((M2,)),
        D, D, D, D, D, D,
        D((2,)), D((2,)), D, D,
        D((4,)), D((4,)), D, D,
    ]
    row = lambda v: v.reshape(1, -1)
    args = (
        latent.T, context, row(cond), row(ctx_cond), w_shift.T, w_scale.T, w_gate.T, row(norm_gain),
        w_query, w_key, w_value, w_decay_fwd, w_decay_bwd, row(forgetting_shift_vector), decay_log.T,
        row(head_gain), w_out,
    )
    out = pl.pallas_call(
        functools.partial(kernel, dims),
        out_shape=jax.ShapeDtypeStruct((64, tok), bf16),
        in_specs=[pl.BlockSpec(memory_space=pl.ANY)] * len(args),
        out_specs=pl.BlockSpec(memory_space=pltpu.VMEM),
        scratch_shapes=scratch,
        compiler_params=pltpu.CompilerParams(
            collective_id=0, has_side_effects=True, vmem_limit_bytes=56 * 1024 * 1024
        ),
        name="mixer",
    )(*args)
    return out.T


def solution(mesh):
    tp = P("tp")
    rows = P("tp", None)
    both = P("sp", "tp")
    return jax.shard_map(
        per_device,
        mesh=mesh,
        in_specs=(
            both, both, P("sp"), P("sp"), both, both, both, tp, rows, rows, rows, rows, rows, tp, both, tp, rows,
        ),
        out_specs=both,
        check_vma=False,
    )
```

```python
import functools
import heapq
from types import SimpleNamespace

import jax
import jax.numpy as jnp
from jax import lax
from jax.experimental import pallas as pl
from jax.experimental.pallas import tpu as pltpu
from jax.sharding import PartitionSpec as P

f32 = jnp.float32
bf16 = jnp.bfloat16
EPS = 1e-06
STREAMS = (("y", 48, 80), ("x", 0, 48))
FEATS = 128


def halves(n, swap):
    small = (n // 2) // 16 * 16
    return (n - small, small) if swap else (small, n - small)


def gather_plan(X, Y, streams, rate, latency=2.0):
    sizes = {"x": X, "y": Y}
    messages = {}

    def ring(part, axis, base, r0, rows, needs):
        n = sizes[axis]
        swap = (sum(base) % 2) == 1
        for sign in (1, -1):
            for hop in range(1, n // 2 + 1):
                a, b = r0, rows
                if 2 * hop == n:
                    first, second = halves(rows, swap)
                    a, b = (r0, first) if sign == 1 else (r0 + first, second)
                offset = list(base)
                offset[0 if axis == "x" else 1] = sign * hop
                before = [(part, axis, base, sign, hop - 1)] if hop > 1 else list(needs)
                messages[(part, axis, base, sign, hop)] = dict(
                    axis=axis, sign=sign, hop=hop, offset=tuple(offset), a=a, n=b, before=before,
                    left=n // 2 - hop + (10 if part[0] == 1 else 0),
                )

    def origins(axis):
        n = sizes[axis]
        return [h for h in range(-(n // 2) + 1, n // 2 + 1)]

    def arrivals(part, axis, base, value):
        n = sizes[axis]
        if value == 0:
            return []
        if 2 * value == n:
            return [(part, axis, base, s, n // 2) for s in (1, -1)]
        return [(part, axis, base, 1 if value > 0 else -1, abs(value))]

    zero = (0, 0)
    for i, (axis, r0, rows) in enumerate(streams):
        ring((1, i), axis, zero, r0, rows, [])
        for v in origins(axis):
            base = (v, 0) if axis == "x" else (0, v)
            ring((2, i), "y" if axis == "x" else "x", base, r0, rows, arrivals((1, i), axis, zero, v))

    return simulate(messages, 768, rate, latency)


def simulate(messages, row_bytes, rate, latency):
    keys = list(messages)
    index = {k: i for i, k in enumerate(keys)}
    free = {(a, s): 0.0 for a in ("x", "y", "all") for s in (1, -1)}
    got, order, started, heap = set(), [], set(), []

    def launch(now):
        ready = [k for k in keys if k not in started and all(b in got for b in messages[k]["before"])]
        ready.sort(key=lambda k: -messages[k]["left"])
        for k in ready:
            m = messages[k]
            link = (m["axis"], m["sign"])
            begin = max(now, free[link])
            hops = m.get("step", 1)
            free[link] = begin + hops * m["n"] * row_bytes / rate
            heapq.heappush(heap, (free[link] + latency + 0.8 * (hops - 1), index[k]))
            started.add(k)
        return [index[k] for k in ready]

    first = launch(0.0)
    steps = []
    while heap:
        now, i = heapq.heappop(heap)
        got.add(keys[i])
        steps.append((i, launch(now), now))
    table = [messages[k] for k in keys]
    return table, first, steps


def share_plan(X, Y, rows, rate, latency=2.0):
    messages = {}
    half = Y // 2
    for v in range(-(X // 2) + 1, X // 2 + 1):
        if v:
            messages[("all", v)] = dict(axis="all", sign=1 if v > 0 else -1, offset=(v, 0), a=0, n=rows, before=[], left=20)
        for sign in (1, -1):
            for hop in range(1, half + 1):
                a, b = 0, rows
                if 2 * hop == Y:
                    first, second = halves(rows, v % 2 == 1)
                    a, b = (0, first) if sign == 1 else (first, second)
                step = 2 if hop % 2 == 0 else 1
                before = [(v, sign, hop - step)] if hop > 2 else [("all", v)] if v else []
                messages[(v, sign, hop)] = dict(
                    axis="y", sign=sign, offset=(v, sign * hop), a=a, n=b, before=before, step=step,
                    left=10 * (half - hop >= 2 and step == 2) + step,
                )
    return simulate(messages, 256, rate, latency)


def rows_done(plan, X, Y):
    table, _, steps = plan
    left = {}
    for m in table:
        oy = m["offset"][1] % Y
        left[oy] = left.get(oy, 0) + 1
    out = []
    for i, _, _ in steps:
        oy = table[i]["offset"][1] % Y
        left[oy] -= 1
        out.append([oy] if left[oy] == 0 else [])
    return out


def split3(v):
    hi = v.astype(bf16)
    r = v - hi.astype(f32)
    mid = r.astype(bf16)
    return hi, mid, (r - mid.astype(f32)).astype(bf16)


def mm(a, b):
    return lax.dot_general(a, b, (((1,), (0,)), ((), ())), preferred_element_type=f32)


def nt(a, b):
    return lax.dot_general(a, b, (((1,), (1,)), ((), ())), preferred_element_type=f32)


def iota(shape, dim):
    return lax.broadcasted_iota(jnp.int32, shape, dim)


def kernel(dims, *refs):
    X, Y, Z, HALF, WIDTH = dims
    NC = X * Y
    TILES = HALF // 128
    NB = 2 * TILES
    GK = X * FEATS
    names = (
        "lat", "ctx", "cond", "cctx", "ws", "wc", "wg", "gain",
        "wq", "wk", "wv", "wf", "wb", "fsv", "dl", "hg",
        "wo", "out", "xg", "xs", "wall", "wog", "gcol", "acc",
        "acc2", "hrow", "hq", "res", "obuf", "ctxo", "ctxp", "ctxm", "ctxg",
        "vec", "fsb", "vecp", "wm", "cnd", "zblk", "zred", "mblk",
        "mrecv", "xyblk", "xyg", "dlv", "pst", "tst",
        "qst", "ost", "zs1", "zs1r", "zmsg", "zrcv", "zent", "ent",
        "cs1", "cs1r", "cmsg", "crcv", "crcv2", "cpk", "loc_sem", "dd_send", "dd_recv",
        "ag1_send", "ag1_recv", "ag2_send", "ag2_recv", "z_send", "z_recv", "xy_send", "xy_recv",
        "cx_send", "cx_recv", "zc_send", "zc_recv", "zl_send", "zl_recv", "wg_send", "wg_recv", "o_send", "o_recv",
    )
    r = SimpleNamespace(**dict(zip(names, refs, strict=True)))

    z = lax.axis_index("sp")
    tp = lax.axis_index("tp")
    c = lax.rem(tp, 2)
    chip = lax.div(tp, 2)
    x = lax.rem(chip, X)
    y = lax.div(chip, X)
    o = 1 - c

    def along_x(step):
        return at(z, lax.rem(x + step + X, X), y, c)

    scopes = []

    def mark(name):
        if scopes:
            scopes.pop().__exit__(None, None, None)
        if name:
            s = jax.named_scope(name)
            s.__enter__()
            scopes.append(s)

    mark("start")

    def at(zz, xx, yy, cc):
        return (zz, (yy * X + xx) * 2 + cc)

    partner = at(z, x, y, o)
    far = lambda d, n: min(d, n - d)
    zstep = sorted(range(1, Z), key=lambda j: -far(j, Z))
    zpeer = [at(lax.rem(z + j, Z), x, y, c) for j in zstep]
    offs = [(dx, dy) for dy in range(Y) for dx in range(X) if dx or dy]
    offs.sort(key=lambda d: -far(d[0], X) - far(d[1], Y))
    xypeer = [at(z, lax.rem(x + dx, X), lax.rem(y + dy, Y), c) for dx, dy in offs]

    def remote(src, dst, ssem, rsem, dev):
        return pltpu.make_async_remote_copy(
            src_ref=src, dst_ref=dst, send_sem=ssem, recv_sem=rsem,
            device_id=dev, device_id_type=pl.DeviceIdType.MESH,
        )

    def wait_sends(ref, ssem, rsem):
        remote(ref, ref, ssem, rsem, partner).wait_send()

    def wait_recvs(ref, ssem, rsem):
        remote(ref, ref, ssem, rsem, partner).wait_recv()

    half = pl.ds(pl.multiple_of(c * HALF, 128), HALF)
    other = pl.ds(pl.multiple_of(o * HALF, 128), HALF)
    wrows = (("wq", 0, 32), ("wk", 64, 32), ("wv", 128, 64), ("wf", 256, 32), ("wb", 320, 32))

    def mine(base, n):
        return pl.ds(pl.multiple_of(base + c * n, 16), n)

    local = []

    def bring(src, dst):
        cp = pltpu.make_async_copy(src, dst, r.loc_sem.at[len(local)])
        cp.start()
        local.append(cp)

    bring(r.cond, r.cnd.at[0])
    bring(r.cctx, r.cnd.at[1])
    bring(r.ws, r.wm.at[0])
    bring(r.wc, r.wm.at[1])
    bring(r.wg, r.wm.at[2])
    bring(r.gain, r.vec.at[0])
    bring(r.hg, r.vec.at[1])
    bring(r.fsv, r.fsb)
    n_first = len(local)
    bring(r.ctx.at[pl.ds(pl.multiple_of(c * 16, 16), 16)], r.ctxo)
    bring(r.lat.at[:, half], r.xg.at[chip, mine(0, 64)])
    n_second = len(local)
    bring(r.dl.at[:, half], r.dlv.at[0])
    for name, base, n in wrows:
        bring(getattr(r, name), r.wall.at[mine(base, n)])
    bring(r.wo, r.wog.at[x, mine(0, 64)])

    barrier = pltpu.get_barrier_semaphore()
    peers = [partner] + xypeer + zpeer
    for dev in peers:
        pl.semaphore_signal(barrier, inc=1, device_id=dev, device_id_type=pl.DeviceIdType.MESH)
    for cp in local[:n_first]:
        cp.wait()

    kw = r.cnd.shape[2]
    row8 = iota((8, kw), 0)
    cl = r.cnd[0]
    cc = r.cnd[1]
    al = (cl * jax.nn.sigmoid(cl)).astype(bf16).astype(f32)
    ac = (cc * jax.nn.sigmoid(cc)).astype(bf16).astype(f32)
    act = jnp.where(row8 == 1, jnp.broadcast_to(ac, (8, kw)), jnp.broadcast_to(al, (8, kw))).astype(bf16)
    d1 = nt(act, jnp.concatenate([r.wm[0], r.wm[1]], axis=0))
    d2 = nt(act, jnp.concatenate([r.wm[2], r.wm[2]], axis=0))
    r8 = iota((8, 128), 0)
    l8 = iota((8, 128), 1)
    part = jnp.where(r8 < 2, d1, d2)
    r.zblk[...] = part
    hg64 = r.vec[1]
    gn64 = r.vec[0]
    hgd = jnp.concatenate([hg64, hg64], axis=1)
    gnd = jnp.concatenate([gn64, gn64], axis=1)
    f1 = r.fsb[...]
    fsd = jnp.concatenate([f1, f1, f1, f1], axis=1)
    vown = jnp.where(r8 == 0, hgd, jnp.where(r8 == 1, fsd, gnd))
    r.mblk[pl.ds(16, 8)] = vown

    mark("barrier")
    pl.semaphore_wait(barrier, len(peers))

    mark("sends")
    for j, dev in enumerate(zpeer):
        cp = remote(r.zblk.at[pl.ds(0, 4)], r.zred.at[z, pl.ds(0, 4)], r.z_send, r.z_recv, dev)
        cp.start()
    dd = []

    def give(src, dst):
        k = len(dd)
        cp = remote(src, dst, r.dd_send.at[k], r.dd_recv.at[k], partner)
        cp.start()
        dd.append(cp)
        return cp

    d_lat = give(r.lat.at[:, other], r.xg.at[chip, mine(0, 64)])
    d_ctx = give(r.ctx.at[pl.ds(pl.multiple_of(o * 16, 16), 16)], r.ctxp)
    for cp in local[n_first:n_second]:
        cp.wait()

    plan = gather_plan(X, Y, STREAMS, 42.0e3, 2.8)
    table = plan[0]

    def gather(plan, buf, ssem, rsem, after):
        table, first, steps = plan
        copies = {}

        def slot_of(ox, oy):
            return lax.rem(y - oy + Y, Y) * X + lax.rem(x - ox + X, X)

        def go(i):
            m = table[i]
            ox, oy = m["offset"]
            if m["axis"] == "all":
                to = lax.rem(x + ox + X, X)
                src = r.hrow.at[pl.ds(pl.multiple_of(to * m["n"], 16), m["n"])]
                dst, dev = buf.at[chip], along_x(ox)
            else:
                if m["axis"] == "x":
                    dev = along_x(m["sign"])
                    slot = slot_of(ox - m["sign"], oy)
                else:
                    step = m["sign"] * m.get("step", 1)
                    dev = at(z, x, lax.rem(y + step + Y, Y), c)
                    slot = slot_of(ox, oy - step)
                src = dst = buf.at[slot, pl.ds(m["a"], m["n"])]
            copies[i] = remote(src, dst, ssem, rsem.at[i], dev)
            copies[i].start()

        for i in first:
            go(i)
        after(-1, 0.0)
        for s, (i, then, when) in enumerate(steps):
            m = table[i]
            ref = buf.at[slot_of(*m["offset"]), pl.ds(m["a"], m["n"])]
            wait_recvs(ref, ssem, rsem.at[i])
            for k in then:
                go(k)
            after(s, when)
        return copies

    lane128 = l8[:1]
    mylane = lane128 // 64 == c

    def join(own, recv, lanes):
        return jnp.where(lanes // 64 == c, own, recv)

    state = {}

    def send_ctx():
        d_ctx.wait_recv()
        own = r.ctxo[...].astype(f32)
        rec = r.ctxp[...].astype(f32)
        lo = jnp.where(c == 0, own, rec)
        hi = jnp.where(c == 0, rec, own)
        both = jnp.concatenate([lo, hi], axis=1).astype(bf16)
        r.ctxm[...] = both
        r.ctxg[chip] = both
        for j, dev in enumerate(xypeer):
            cp = remote(r.ctxm, r.ctxg.at[chip], r.cx_send, r.cx_recv, dev)
            cp.start()

    def send_weights():
        state["wd1"] = [give(getattr(r, name), r.wall.at[mine(base, n)]) for name, base, n in wrows]
        state["wd1"].append(give(r.dl.at[:, other], r.dlv.at[1]))
        state["wd1"].append(give(r.wo, r.wog.at[x, mine(0, 64)]))

    def z_sum():
        wait_recvs(r.zred.at[pl.ds(0, Z - 1), pl.ds(0, 4)], r.z_send, r.z_recv)
        r.zred[z] = part
        M = r.zred[0][0:4]
        for j in range(1, Z):
            M = M + r.zred[j][0:4]
        M = jnp.concatenate([M, M], axis=0)
        rM = pltpu.roll(M, 64, 1)
        r.mblk[pl.ds(0, 8)] = jnp.where(l8 < 64, M, rM)
        r.mblk[pl.ds(8, 8)] = jnp.where(l8 < 64, rM, M)
        state["mod"] = give(r.mblk, r.mrecv)

    def xy_send():
        state["mod"].wait_recv()
        lanes = iota((24, 128), 1)
        rws = iota((24, 128), 0)
        pick = jnp.where(rws == 17, (lanes // 32) % 2, lanes // 64)
        both = jnp.where(pick == c, r.mblk[...], r.mrecv[...])
        A = both[0:8]
        B = both[8:16]
        V = both[16:24]
        r.vecp[...] = jnp.where(r8 < 2, V, jnp.where(r8 == 2, A, 0.0))
        G = V[2:3] * (1.0 + B)
        blk = jnp.where(r8 < 2, A, jnp.where(r8 < 4, pltpu.roll(G, 2, 0), pltpu.roll(A, 2, 0)))
        r.xyblk[...] = blk
        r.xyg[chip] = blk
        for j, dev in enumerate(xypeer):
            cp = remote(r.xyblk, r.xyg.at[chip], r.xy_send, r.xy_recv, dev)
            cp.start()

    def w_part(slot, a, n):
        return r.wog.at[lax.rem(slot + X, X), pl.ds(pl.multiple_of(c * 64 + a, 16), n)]

    wg = []

    def w_ring(sign, slot, a, n):
        k = len(wg)
        ref = w_part(slot, a, n)
        cp = remote(ref, ref, r.wg_send.at[k], r.wg_recv.at[k], along_x(sign))
        cp.start()
        wg.append((cp, slot - sign, a, n))

    def w_landed(k):
        _, slot, a, n = wg[k]
        ref = w_part(slot, a, n)
        remote(ref, ref, r.wg_send.at[k], r.wg_recv.at[k], partner).wait_recv()
        return give(ref, ref)

    def w_first():
        if X == 2:
            w_ring(1, x, 0, 32)
            w_ring(-1, x, 32, 32)
        else:
            w_ring(1, x, 0, 64)
            w_ring(-1, x, 0, 64)

    def w_second():
        state["wd"] = [w_landed(0), w_landed(1)]
        if X == 4:
            w_ring(1, x - 1, 0, 32)
            w_ring(-1, x + 1, 32, 32)

    def w_third():
        if X == 4:
            state["wd"] += [w_landed(2), w_landed(3)]
        for cp in state["wd"]:
            cp.wait_recv()

    def cols_of(v):
        return jnp.transpose(jnp.concatenate([v, jnp.zeros((120, 128), f32)], axis=0))

    row128 = iota((128, 128), 0)
    ln128 = iota((128, 128), 1)
    same = (row128 // 64) == (ln128 // 64)
    tri = jnp.where(same & (row128 <= ln128), 1.0, 0.0).astype(bf16)
    blk_ones = jnp.where(same, 1.0, 0.0).astype(bf16)
    sums = jnp.concatenate([tri, blk_ones], axis=1)
    ind = jnp.where((r8 < 2) & (l8 // 64 == r8), 1.0, 0.0).astype(bf16)
    head_lane = (lane128 // 32) % 2
    mf = same & (row128 <= ln128)
    mb = same & (row128 >= ln128)

    def exponents(L):
        hi, mid, lo = split3(L)
        big = mm(jnp.concatenate([hi, mid, lo], axis=0), sums)
        big = big[0:128] + big[128:256] + big[256:384]
        C, T = big[:, 0:128], big[:, 128:256]
        E = jnp.where(row128 < 64, C, T - C + L)
        tot = nt(ind, hi) + nt(ind, mid) + nt(ind, lo)
        return E, T - E, tot

    def terms(k2, vT, D):
        ks = k2 * jnp.exp(D)
        stack = jnp.concatenate(
            [jnp.where(ln128 < 64, ks, 0.0).astype(bf16), jnp.where(ln128 < 64, 0.0, ks).astype(bf16)], axis=0
        )
        K = nt(vT, stack)
        first = jnp.where(head_lane == 0, K[0:64, 0:128], K[64:128, 0:128])
        second = jnp.where(head_lane == 0, K[0:64, 128:256], K[64:128, 128:256])
        return first, second

    def log_sigmoid(v):
        return jnp.minimum(v, 0.0) - jnp.log1p(jnp.exp(-jnp.abs(v)))

    lane64 = iota((64, 128), 1)
    lane32 = iota((32, 128), 1)
    lane16 = iota((16, 128), 1)

    def chip_state(stage, recv, own_ref):
        own = own_ref[pl.ds(pl.multiple_of(c * 32, 8), 32)]
        rec = recv[pl.ds(0, 32)]
        town = stage[pl.ds(32, 1)]
        trec = recv[pl.ds(32, 1)]
        s0 = jnp.where(c == 0, own, rec)
        s1 = jnp.where(c == 0, rec, own)
        t0 = jnp.where(c == 0, town, trec)
        t1 = jnp.where(c == 0, trec, town)
        both = jnp.where(lane32 < 64, jnp.exp(t1) * s0 + s1, jnp.exp(t0) * s1 + s0)
        return both, t0, t1, s0, s1

    def log_rows(T):
        hi = T.astype(bf16).astype(f32)
        return jnp.where(iota((16, 128), 0) == 0, hi, jnp.where(iota((16, 128), 0) == 1, T - hi, 0.0))

    def mod_in():
        wait_recvs(r.xyg.at[pl.ds(0, NC - 1)], r.xy_send, r.xy_recv)
        wait_recvs(r.ctxg.at[pl.ds(0, NC - 1)], r.cx_send, r.cx_recv)
        for cp in local[n_second:]:
            cp.wait()
        for cp in state["wd1"]:
            cp.wait_recv()

        for q in range(max(NC // 16, 1)):
            n = min(NC, 16)
            rows = r.xyg[pl.ds(q * n, n)].reshape(n * 8, 128)
            if n < 16:
                rows = jnp.concatenate([rows, jnp.zeros((128 - n * 8, 128), f32)], axis=0)
            t = jnp.transpose(rows)
            for b in range(n):
                r.gcol[q * n + b] = jnp.broadcast_to(t[:, b * 8 + 2 : b * 8 + 3], (128, 128))

    def ctx_work(sq):
        pcv = r.acc[:, pl.ds(HALF, 128)]
        sqt = jnp.transpose(jnp.concatenate([sq, jnp.zeros((112, 128), f32)], axis=0))
        ssum = jnp.sum(sqt, axis=0, keepdims=True)
        inv = lax.rsqrt(ssum / WIDTH + EPS)
        cp_ = inv * pcv + pcv[:, 17:18]
        valid = ln128 < 16
        k = jnp.where(valid[0:64], cp_[64:128], 0.0).astype(bf16).astype(f32)
        k2 = jnp.concatenate([k, k], axis=0)
        vT = jnp.where(valid, cp_[128:256], 0.0).astype(bf16)
        colv = cols_of(r.vecp[...])
        L = jnp.where(valid, log_sigmoid(cp_[256:384] + colv[:, 1:2]) / 16.0, 0.0)
        E, D, tot = exponents(L)
        first, _ = terms(k2, vT, D)
        r.cpk[...] = first
        r.cs1[pl.ds(0, 32)] = jnp.where(c == 0, first[32:64], first[0:32])
        r.cs1[pl.ds(32, 8)] = jnp.broadcast_to(tot[0:1], (8, 128))
        state["c1"] = give(r.cs1, r.cs1r)

    G = min(4, Z)
    za, zb = lax.div(z, G), lax.rem(z, G)

    def ctx_message(both, T):
        return jnp.concatenate([both, log_rows(T)[0:8]], axis=0).astype(bf16)

    def ctx_fold(ref, n):
        sf = sb = T = None
        for i in range(n):
            m = ref[i].astype(f32)
            t = m[32:33] + m[33:34]
            sf = m[0:32] if i == 0 else jnp.exp(t) * sf + m[0:32]
            T = t if i == 0 else T + t
            m = ref[n - 1 - i].astype(f32)
            sb = m[0:32] if i == 0 else jnp.exp(m[32:33] + m[33:34]) * sb + m[0:32]
        return jnp.where(lane32 < 64, sf, sb), T

    def ctx_send():
        state["c1"].wait_recv()
        both, t0, t1, _, _ = chip_state(r.cs1, r.cs1r, r.cpk)
        msg = ctx_message(both, t0 + t1)
        r.cmsg[0] = msg
        r.crcv[zb] = msg
        for j in range(1, G):
            dev = at(za * G + lax.rem(zb + j, G), x, y, c)
            cp = remote(r.cmsg.at[0], r.crcv.at[zb], r.zc_send.at[0], r.zc_recv.at[0], dev)
            cp.start()

    def ctx_second():
        wait_recvs(r.crcv.at[pl.ds(0, G - 1)], r.zc_send.at[0], r.zc_recv.at[0])
        both, T = ctx_fold(r.crcv, G)
        msg = ctx_message(both, T)
        r.cmsg[1] = msg
        r.crcv2[za] = msg
        for j in range(1, Z // G):
            dev = at(lax.rem(z + j * G, Z), x, y, c)
            cp = remote(r.cmsg.at[1], r.crcv2.at[za], r.zc_send.at[1], r.zc_recv.at[1], dev)
            cp.start()

    def ctx_done():
        if Z > G:
            wait_recvs(r.crcv2.at[pl.ds(0, Z // G - 1)], r.zc_send.at[1], r.zc_recv.at[1])
        r.cpk[pl.ds(0, 32)] = ctx_fold(r.crcv2, Z // G)[0]

    sums_of = {"lat": [jnp.zeros((8, 128), f32) for _ in range(TILES)], "ctx": jnp.zeros((16, 128), f32), "n": 0}

    def project(yy):
        for xx in range(X):
            b = yy * X + xx
            xr = pl.ds(xx * 128, 128)
            for t in range(TILES):
                v = r.xg[b, :, pl.ds(t * 128, 128)].astype(f32)
                s2 = v * v
                part_s = s2[0:8]
                for q in range(1, 16):
                    part_s = part_s + s2[q * 8 : q * 8 + 8]
                sums_of["lat"][t] = sums_of["lat"][t] + part_s
                r.xs[xr, pl.ds(t * 128, 128)] = (v * r.gcol[b]).astype(bf16)
            m = r.xyg[b]
            raw = r.ctxg[b].astype(f32)
            sums_of["ctx"] = sums_of["ctx"] + raw * raw
            rows = jnp.concatenate([raw * m[3:4], m, jnp.zeros((104, 128), f32)], axis=0)
            r.xs[xr, pl.ds(HALF, 128)] = jnp.transpose(rows).astype(bf16)
        step = mm(r.wall[:, pl.ds(pl.multiple_of(yy * GK, 128), GK)], r.xs[...])
        r.acc[...] = step if sums_of["n"] == 0 else r.acc[...] + step
        sums_of["n"] += 1

    actions = [(9.5, z_sum), (10.3, xy_send), (10.8, send_ctx), (12.0, send_weights)]
    pending = list(actions)
    rows1 = rows_done(plan, X, Y)
    last_go = max(i for i, st in enumerate(plan[2]) if st[1])
    waiting = []

    def after1(s, when):
        if s < 0:
            return
        while pending and pending[0][0] <= when:
            fn = pending.pop(0)[1]
            with jax.named_scope(fn.__name__):
                fn()
        waiting.extend(rows1[s])
        if s == last_go:
            while pending:
                pending.pop(0)[1]()
            with jax.named_scope("mod_in"):
                mod_in()
            w_first()
        if s >= last_go:
            while waiting:
                with jax.named_scope("project"):
                    project(lax.rem(y - waiting.pop(0) + Y, Y))

    mark("d_lat")
    d_lat.wait_recv()
    mark("ag1")
    copies1 = gather(plan, r.xg, r.ag1_send, r.ag1_recv, after1)
    ss = sums_of["lat"]

    mark("attend")
    colv = cols_of(r.vecp[...])
    shift_col = r.acc[:, pl.ds(HALF, 128)][:, 16:17]
    own_dl = r.dlv[0]
    rec_dl = r.dlv[1]
    dl0 = jnp.where(c == 0, own_dl, rec_dl)
    dl1 = jnp.where(c == 0, rec_dl, own_dl)
    for t in range(TILES):
        ts = pl.ds(t * 128, 128)
        inv = lax.rsqrt(jnp.sum(ss[t], axis=0, keepdims=True) / WIDTH + EPS)
        pr = inv * r.acc[:, ts] + shift_col
        q = pr[0:64].astype(bf16).astype(f32) * (32.0 ** -0.5)
        k = pr[64:128].astype(bf16).astype(f32)
        vT = pr[128:256].astype(bf16)
        q2 = jnp.concatenate([q, q], axis=0)
        k2 = jnp.concatenate([k, k], axis=0)
        dlt = jnp.where((row128 // 32) % 2 == 0, dl0[:, t * 128 : t * 128 + 128], dl1[:, t * 128 : t * 128 + 128])
        L = log_sigmoid(pr[256:384] + colv[:, 1:2]) / 16.0 + dlt
        E, D, tot = exponents(L)
        first, second = terms(k2, vT, D)
        r.pst[2 * t] = first
        r.pst[2 * t + 1] = second
        r.tst[t] = tot
        qf = q2 * jnp.exp(E)
        r.qst[t] = qf
        r.ost[t, 0] = k2 * jnp.exp(-E)
        r.ost[t, 1] = vT.astype(f32)

    T = [r.tst[i // 2][i % 2 : i % 2 + 1] for i in range(NB)]
    e = [jnp.exp(v) for v in T]
    sf = jnp.zeros((64, 128), f32)
    sb = jnp.zeros((64, 128), f32)
    for i in range(NB):
        sf = e[i] * sf + r.pst[i]
        sb = e[NB - 1 - i] * sb + r.pst[NB - 1 - i]
    seg = jnp.where(lane64 < 64, sf, sb)
    tseg = sum(T[1:], T[0])
    r.zent[...] = seg
    r.zs1[pl.ds(0, 32)] = jnp.where(c == 0, seg[32:64], seg[0:32])
    r.zs1[pl.ds(32, 8)] = jnp.broadcast_to(tseg, (8, 128))
    d_seg = give(r.zs1, r.zs1r)
    mark("ctx_work")
    ctx_work(sums_of["ctx"])
    mark("d_seg")
    ctx_send()
    d_seg.wait_recv()
    mark("combine")
    both, t0, t1, s0, s1 = chip_state(r.zs1, r.zs1r, r.zent)
    tc = t0 + t1
    rtc = pltpu.roll(jnp.broadcast_to(tc, (8, 128)), 64, 1)[0:1]
    ra = pltpu.roll(both[0:16], 64, 1)
    rb = pltpu.roll(both[16:32], 64, 1)
    r.zmsg[0] = jnp.concatenate(
        [jnp.where(lane16 < 64, both[0:16], rb), log_rows(jnp.where(lane128 < 64, tc, rtc))[0:8]], axis=0
    ).astype(bf16)
    r.zmsg[1] = jnp.concatenate(
        [jnp.where(lane16 < 64, ra, both[16:32]), log_rows(jnp.where(lane128 < 64, rtc, tc))[0:8]], axis=0
    ).astype(bf16)
    r.zrcv[z] = jnp.zeros((24, 128), bf16)
    for j, dev in enumerate(zpeer):
        behind = jnp.where(z + zstep[j] >= Z, 1, 0)
        cp = remote(r.zmsg.at[behind], r.zrcv.at[z], r.zl_send, r.zl_recv, dev)
        cp.start()

    mark("scores")
    for t in range(TILES):
        qf = r.qst[t]
        kdT = jnp.transpose(r.ost[t, 0]).astype(bf16)
        vT = r.ost[t, 1].astype(bf16)
        parts = [jnp.where(row128 // 32 == i, qf, 0.0).astype(bf16) for i in range(4)]
        AT = mm(kdT, jnp.concatenate(parts, axis=1))
        A0 = jnp.where(mf, AT[:, 0:128], 0.0) + jnp.where(mb, AT[:, 256:384], 0.0)
        A1 = jnp.where(mf, AT[:, 128:256], 0.0) + jnp.where(mb, AT[:, 384:512], 0.0)
        r.ost[t, 1] = jnp.concatenate(
            [mm(vT[0:64], A0.astype(bf16)), mm(vT[64:128], A1.astype(bf16))], axis=0
        )

    mark("ctx_second")
    ctx_second()
    mark("w_second")
    w_second()
    mark("ctx_done")
    ctx_done()
    mark("zwait")
    wait_recvs(r.zrcv.at[pl.ds(0, Z - 1)], r.zl_send, r.zl_recv)
    mark("entering")
    ctxs = r.cpk[pl.ds(0, 32)]
    ca = pltpu.roll(ctxs[0:16], 64, 1)
    cb = pltpu.roll(ctxs[16:32], 64, 1)
    ef = jnp.where(lane16 < 64, ctxs[0:16], cb)
    eb = jnp.where(lane16 < 64, ca, ctxs[16:32])
    for s in range(Z):
        m = r.zrcv[s].astype(f32)
        ef = jnp.where(s < z, jnp.exp(m[16:17] + m[17:18]) * ef + m[0:16], ef)
        u = Z - 1 - s
        m = r.zrcv[u].astype(f32)
        eb = jnp.where(u > z, jnp.exp(m[16:17] + m[17:18]) * eb + m[0:16], eb)
    ech = jnp.concatenate(
        [
            jnp.where(lane16 < 64, ef, pltpu.roll(eb, 64, 1)),
            jnp.where(lane16 < 64, pltpu.roll(ef, 64, 1), eb),
        ],
        axis=0,
    )
    ent0 = jnp.where(lane32 < 64, ech, jnp.exp(t1) * ech + s1)
    ent1 = jnp.where(lane32 < 64, jnp.exp(t0) * ech + s0, ech)
    rows_c = pl.ds(pl.multiple_of(c * 32, 8), 32)
    d_seg.wait_send()
    r.zs1[pl.ds(0, 32)] = jnp.where(c == 0, ent1, ent0)
    r.ent[rows_c] = jnp.where(c == 0, ent0, ent1)
    mark("d_ent")
    d_ent = give(r.zs1.at[pl.ds(0, 32)], r.ent.at[rows_c])
    d_ent.wait_recv()

    mark("post")
    sf = r.ent[...]
    sb = sf
    fin, bin_ = [None] * NB, [None] * NB
    for i in range(NB):
        fin[i] = sf
        sf = e[i] * sf + r.pst[i]
        u = NB - 1 - i
        bin_[u] = sb
        sb = e[u] * sb + r.pst[u]
    hcol = colv[:, 0:1]
    for t in range(TILES):
        qf = r.qst[t]
        lhs = []
        for i in (2 * t, 2 * t + 1):
            s_in = jnp.where(lane64 < 64, fin[i], bin_[i])
            lhs.append(
                jnp.concatenate(
                    [jnp.where(head_lane == 0, s_in, 0.0), jnp.where(head_lane == 1, s_in, 0.0)], axis=0
                ).astype(bf16)
            )
        rhs = jnp.concatenate(
            [jnp.where(ln128 < 64, qf, 0.0).astype(bf16), jnp.where(ln128 < 64, 0.0, qf).astype(bf16)], axis=0
        )
        mixed = r.ost[t, 1] + mm(jnp.concatenate(lhs, axis=1), rhs)
        outs = []
        for h in range(2):
            mh = mixed[h * 64 : h * 64 + 64]
            outs.append(mh * lax.rsqrt(jnp.mean(mh * mh, axis=0, keepdims=True) + EPS))
        heads = jnp.concatenate(outs, axis=0) * hcol
        r.hrow[pl.ds(t * 128, 128)] = jnp.transpose(heads).astype(bf16)

    mark("ag2")
    TQ = HALF // X
    plan2 = share_plan(X, Y, TQ, 46.0e3, 2.8)
    r.hq[chip] = r.hrow[pl.ds(pl.multiple_of(x * TQ, 16), TQ)]
    done2 = rows_done(plan2, X, Y)
    ready2 = []

    def product(yy):
        heads = jnp.concatenate([r.hq[yy * X + xx] for xx in range(X)], axis=1)
        ks = pl.ds(pl.multiple_of(yy * GK, 128), GK)
        step = nt(r.wog[:, :, ks].reshape(X * 128, GK), heads)
        r.acc2[...] = step if not ready2 else r.acc2[...] + step
        ready2.append(yy)

    w_at = max([i for i, st in enumerate(plan2[2]) if st[1]], default=0)
    waiting2 = []

    def after2(s, when):
        if s < 0:
            return
        waiting2.extend(done2[s])
        if s == w_at:
            with jax.named_scope("w_third"):
                w_third()
        if s >= w_at:
            while waiting2:
                product(lax.rem(y - waiting2.pop(0) + Y, Y))

    copies2 = gather(plan2, r.hq, r.ag2_send, r.ag2_recv, after2)
    mark("final")
    gates = jnp.concatenate([r.xyg[y * X + xx][4:5] for xx in range(X)] + [jnp.zeros((8 - X, 128), f32)], axis=0)
    gates = cols_of(gates)
    for xx in range(X):
        piece = (r.acc2[pl.ds(xx * 128, 128)] * gates[:, xx : xx + 1]).astype(bf16)
        r.res[xx, 0] = piece[0:64]
        r.res[xx, 1] = piece[64:128]
    mine_at = 2 * x + c
    for dx, dc in [(dx, dc) for dx in (2, 1, 3, 0) if dx < X for dc in (0, 1) if dx or dc]:
        tx = lax.rem(x + dx, X)
        tc_ = lax.rem(c + dc, 2)
        cp = remote(
            r.res.at[tx, tc_], r.obuf.at[mine_at], r.o_send, r.o_recv, at(z, tx, y, tc_)
        )
        cp.start()
    r.obuf[mine_at] = r.res[x, c]
    wait_recvs(r.obuf.at[pl.ds(0, 2 * X - 1)], r.o_send, r.o_recv)
    r.out[...] = jnp.concatenate([r.obuf[2 * xx + cc_] for cc_ in (0, 1) for xx in range(X)], axis=1)
    mark("drain")
    for cp2 in dd:
        if cp2 is not d_seg:
            cp2.wait_send()
    wait_sends(r.zred.at[pl.ds(0, Z - 1), pl.ds(0, 4)], r.z_send, r.z_recv)
    wait_sends(r.ctxg.at[pl.ds(0, NC - 1)], r.cx_send, r.cx_recv)
    wait_sends(r.xyg.at[pl.ds(0, NC - 1)], r.xy_send, r.xy_recv)
    wait_sends(r.crcv.at[pl.ds(0, G - 1)], r.zc_send.at[0], r.zc_recv.at[0])
    if Z > G:
        wait_sends(r.crcv2.at[pl.ds(0, Z // G - 1)], r.zc_send.at[1], r.zc_recv.at[1])
    wait_sends(r.zrcv.at[pl.ds(0, Z - 1)], r.zl_send, r.zl_recv)
    wait_sends(r.obuf.at[pl.ds(0, 2 * X - 1)], r.o_send, r.o_recv)
    for cp2, _, _, _ in wg:
        cp2.wait_send()
    wait_sends(r.xg.at[pl.ds(0, NC - 1)], r.ag1_send, r.ag1_recv.at[0])
    wait_sends(r.hq.at[pl.ds(0, NC - 1)], r.ag2_send, r.ag2_recv.at[0])
    mark(None)


def per_device(
    latent, context, cond, ctx_cond, w_shift, w_scale, w_gate, norm_gain, w_query, w_key, w_value,
    w_decay_fwd, w_decay_bwd, forgetting_shift_vector, decay_log, head_gain, w_out,
):
    Z = lax.axis_size("sp")
    NC = lax.axis_size("tp") // 2
    X = 4 if NC >= 8 else 2
    Y = NC // X
    tok = latent.shape[0]
    HALF = tok // 2
    WIDTH = w_out.shape[1]
    dims = (X, Y, Z, HALF, WIDTH)
    TILES = HALF // 128
    M = len(gather_plan(X, Y, STREAMS, 46.0e3)[0])
    M2 = len(share_plan(X, Y, HALF // X, 46.0e3)[0])
    V = pltpu.VMEM
    D = pltpu.SemaphoreType.DMA
    GK = X * FEATS
    kw = cond.shape[0]
    scratch = [
        V((NC, 128, HALF), bf16),
        V((GK, HALF + 128), bf16),
        V((384, WIDTH), bf16),
        V((X, 128, WIDTH), bf16),
        V((NC, 128, 128), f32),
        V((384, HALF + 128), f32),
        V((X * 128, HALF // X), f32),
        V((HALF, 128), bf16),
        V((NC, HALF // X, 128), bf16),
        V((X, 2, 64, HALF // X), bf16),
        V((2 * X, 64, HALF // X), bf16),
        V((16, 64), bf16),
        V((16, 64), bf16),
        V((16, 128), bf16),
        V((NC, 16, 128), bf16),
        V((2, 1, 64), f32),
        V((1, 32), f32),
        V((8, 128), f32),
        V((3, 64, kw), bf16),
        V((2, 1, kw), f32),
        V((8, 128), f32),
        V((Z, 8, 128), f32),
        V((24, 128), f32),
        V((24, 128), f32),
        V((8, 128), f32),
        V((NC, 8, 128), f32),
        V((2, 1, HALF), f32),
        V((2 * TILES, 64, 128), f32),
        V((TILES, 8, 128), f32),
        V((TILES, 128, 128), f32),
        V((TILES, 2, 128, 128), f32),
        V((40, 128), f32),
        V((40, 128), f32),
        V((2, 24, 128), bf16),
        V((Z, 24, 128), bf16),
        V((64, 128), f32),
        V((64, 128), f32),
        V((40, 128), f32),
        V((40, 128), f32),
        V((2, 40, 128), bf16),
        V((4, 40, 128), bf16),
        V((4, 40, 128), bf16),
        V((64, 128), f32),
        D((17,)), D((17,)), D((17,)),
        D, D((M,)), D, D((M2,)),
        D, D, D, D, D, D,
        D((2,)), D((2,)), D, D,
        D((4,)), D((4,)), D, D,
    ]
    row = lambda v: v.reshape(1, -1)
    args = (
        latent.T, context, row(cond), row(ctx_cond), w_shift.T, w_scale.T, w_gate.T, row(norm_gain),
        w_query, w_key, w_value, w_decay_fwd, w_decay_bwd, row(forgetting_shift_vector), decay_log.T,
        row(head_gain), w_out,
    )
    out = pl.pallas_call(
        functools.partial(kernel, dims),
        out_shape=jax.ShapeDtypeStruct((64, tok), bf16),
        in_specs=[pl.BlockSpec(memory_space=pl.ANY)] * len(args),
        out_specs=pl.BlockSpec(memory_space=pltpu.VMEM),
        scratch_shapes=scratch,
        compiler_params=pltpu.CompilerParams(
            collective_id=0, has_side_effects=True, vmem_limit_bytes=56 * 1024 * 1024
        ),
        name="mixer",
    )(*args)
    return out.T


def solution(mesh):
    tp = P("tp")
    rows = P("tp", None)
    both = P("sp", "tp")
    return jax.shard_map(
        per_device,
        mesh=mesh,
        in_specs=(
            both, both, P("sp"), P("sp"), both, both, both, tp, rows, rows, rows, rows, rows, tp, both, tp, rows,
        ),
        out_specs=both,
        check_vma=False,
    )
```
